32 devices in a mesh: gr: 2 (over x), fs: 8 (over z, y), tp: 2 (over core).
Axes of the slice: x: 2, y: 2, z: 4, core: 2. Of those that a mesh axis runs over, the one named last changes fastest.
Arguments:
- tokens: bfloat16 [4096, 2048], P(('gr', 'tp'), 'fs'), may hold values from -400 to 400
- norm_gain: float32 [2048], P('fs'), may hold values from 0.1 to 1.9
- up_weight: float32 [2048, 8192], P('fs', ('gr', 'tp')), may hold values from -0.125 to 0.125
- down_weight: float32 [8192, 2048], P('fs', ('gr', 'tp')), may hold values from -0.09375 to 0.09375
Outputs:
- mixed: bfloat16 [2048, 4096], P('fs', ('gr', 'tp'))
- up_ready: bfloat16 [2048, 8192], P(None, 'fs')
- down_ready: bfloat16 [8192, 2048], P('fs')
The draws below stay inside these ranges and needn't reach their ends.
All inputs are finite; a program needn't handle non-finite values.
Results may differ from the reference program's by a relative error of at most 0.023.
Values may be sent and summed in bfloat16 or wider, within the bound.
No kernel may reach another device: no remote copies, remote signals or barrier semaphores. Data moves between devices by JAX's collectives and lax.ppermute only.
A program may use at most 64 MiB of HBM per device.

```python
import math
import jax
import jax.numpy as jnp
from jax import lax

D = 2048
FF = 8192
TOKENS = 4096
N_FS = 8


def draw_tokens(key, part):
    keys = jax.random.split(key, 3)
    row_scales = jnp.exp(jax.random.uniform(keys[0], (TOKENS, 1), jnp.float32) * math.log(10.0))
    column_scales = jnp.exp(jax.random.uniform(keys[1], (1, D), jnp.float32) * math.log(10.0))
    base = jax.random.truncated_normal(keys[2], -4.0, 4.0, (TOKENS, D), jnp.float32)
    return (base * row_scales * column_scales).astype(jnp.bfloat16)


def with_spikes(array, key, source, target, shards_of, factor):
    def block_of(axis_at):
        return (jnp.arange(array.shape[axis_at]) // (array.shape[axis_at] // shards_of)).reshape((-1,) + (1,) * (array.ndim - 1 - axis_at))

    one_side = jax.random.permutation(key, shards_of)[block_of(target)]
    other_side = (block_of(target) + shards_of // 2) % shards_of
    return jnp.where((block_of(source) == one_side) | (block_of(source) == other_side), factor * array, array)


def steps_of(own_key, shape, shards, least, largest):
    def one(position, parts):
        draws = jax.random.uniform(jax.random.fold_in(jax.random.fold_in(own_key, 6), position), (parts,), jnp.float32, least / len(shards), largest / len(shards))
        return jnp.repeat(jnp.exp(draws), shape[position] // parts).reshape((-1,) + (1,) * (len(shape) - position - 1))

    factor_of = one(*shards[0])
    for cut in shards[1:]:
        factor_of = factor_of * one(*cut)
    return factor_of


def scatter_about(stream_key, shape, scale, most, pieces=(), kind=jnp.bfloat16):
    drawn = jax.random.normal(stream_key, shape, jnp.float32) * scale
    if len(pieces) > 0:
        drawn = steps_of(stream_key, shape, pieces, -0.22, 0.18) * drawn
    return jnp.clip(drawn, min=-most, max=most).astype(kind)


def gaussian_with(own_key, shape, scale, bound, cuts, heavy, kind=jnp.bfloat16):
    entries = scale * jax.random.normal(own_key, shape, jnp.float32)
    if cuts:
        entries = entries * steps_of(own_key, shape, cuts, -0.22, 0.18)
    return jnp.clip(with_spikes(entries, jax.random.fold_in(own_key, 3), *heavy), -bound, bound).astype(kind)


def setup_inputs(seed: int = 0) -> dict:
    arg_keys = jax.random.split(jax.random.key(seed), 5)
    return {
        "tokens": draw_tokens(jax.random.fold_in(arg_keys[4], 71), 0),
        "norm_gain": jnp.clip(1.0 + 0.18 * jax.random.normal(arg_keys[1], (D,), jnp.float32), 0.1, 1.9),
        "up_weight": scatter_about(arg_keys[2], (D, FF), D ** -0.5, 0.125, ((0, 8), (1, 4)), jnp.float32),
        "down_weight": gaussian_with(arg_keys[3], (FF, D), FF ** -0.5, 0.09375, ((0, 8), (1, 4)), (0, 1, 8, 2.0), jnp.float32),
    }


epsilon = 1e-06

def reference(tokens, norm_gain, up_weight, down_weight):
    up_ready = (norm_gain[:, None] * up_weight).astype(jnp.bfloat16)
    down_ready = down_weight.astype(jnp.bfloat16)
    raw_up = jnp.dot(tokens, up_ready, preferred_element_type=jnp.float32)
    widened = tokens.astype(jnp.float32)
    row_scale = lax.rsqrt(lax.optimization_barrier(jnp.mean(widened * widened, axis=1)) + epsilon)
    hidden = jnp.square(jax.nn.relu(raw_up * row_scale[:, None])).astype(jnp.bfloat16)
    block = FF // N_FS

    def add_block(running, index):
        start = (index * block).astype(jnp.int32)
        piece = lax.dynamic_slice_in_dim(hidden, start, block, 1)
        weight_rows = lax.dynamic_slice_in_dim(down_ready, start, block, 0)
        partial_value = jnp.dot(piece, weight_rows, preferred_element_type=jnp.float32).astype(jnp.bfloat16)
        partial_value = lax.optimization_barrier(partial_value).astype(jnp.float32)
        return (running + partial_value, None)
    running, _ = lax.scan(add_block, jnp.zeros((TOKENS, D), jnp.float32), jnp.arange(N_FS, dtype=jnp.int32))
    return (running.T.astype(jnp.bfloat16), up_ready, down_ready)
```

```python
import math

import jax
import jax.numpy as jnp
from jax import lax
from jax.experimental import pallas as pl
from jax.experimental.pallas import tpu as pltpu
from jax.sharding import PartitionSpec as P

epsilon = 1e-06


def ring_order(count):
    outer = math.gcd(count, 4)
    inner = count // outer
    if outer % 2 or inner < 2:
        return list(range(count))
    walk = []
    for o in range(outer):
        cols = range(1, inner) if o % 2 == 0 else range(inner - 1, 0, -1)
        walk += [o * inner + i for i in cols]
    return walk + [o * inner for o in range(outer - 1, -1, -1)]


def place(shape, parts):
    arrays, index_of = [], {}
    for part in parts:
        if id(part[0]) not in index_of:
            index_of[id(part[0])] = len(arrays)
            arrays.append(part[0])
    dtype = arrays[0].dtype
    if any(p[2] % 16 or p[1] % 16 or p[0].shape[1] % 128 for p in parts):
        out = jnp.zeros(shape, dtype)
        for array, source, rows, row, col in parts:
            out = lax.dynamic_update_slice(out, array[source : source + rows], (row, col))
        return out
    offsets = jnp.stack([jnp.asarray(o, jnp.int32) for p in parts for o in (p[3], p[4])])
    count = len(parts)

    def kernel(offset_ref, *refs):
        out_ref, sems = refs[-2], refs[-1]

        def copy(n):
            array, source, rows, _, _ = parts[n]
            row = pl.multiple_of(offset_ref[2 * n], 16)
            col = pl.multiple_of(offset_ref[2 * n + 1], 128)
            return pltpu.make_async_copy(
                refs[index_of[id(array)]].at[pl.ds(source, rows), :],
                out_ref.at[pl.ds(row, rows), pl.ds(col, array.shape[1])],
                sems.at[n],
            )

        for n in range(count):
            copy(n).start()
        for n in range(count):
            copy(n).wait()

    return pl.pallas_call(
        kernel,
        out_shape=jax.ShapeDtypeStruct(shape, dtype),
        in_specs=[pl.BlockSpec(memory_space=pltpu.SMEM)] + [pl.BlockSpec(memory_space=pl.ANY)] * len(arrays),
        out_specs=pl.BlockSpec(memory_space=pl.ANY),
        scratch_shapes=[pltpu.SemaphoreType.DMA((count,))],
    )(offsets, *arrays)


def shards(tokens, norm_gain, up_weight, down_weight):
    fs_count = lax.axis_size("fs")
    gr_count, tp_count = lax.axis_size("gr"), lax.axis_size("tp")
    group_count = gr_count * tp_count
    f, g, t = lax.axis_index("fs"), lax.axis_index("gr"), lax.axis_index("tp")
    c = g * tp_count + t
    order = ring_order(fs_count)
    spot_of = jnp.asarray([order.index(n) for n in range(fs_count)], jnp.int32)
    order_array = jnp.asarray(order, jnp.int32)
    q = spot_of[f]

    def at_ring(shift):
        return order_array[(q + shift) % fs_count]

    def ring_shift(array, by):
        return lax.ppermute(array, "fs", [(order[n], order[(n + by) % fs_count]) for n in range(fs_count)])

    def shift(array, axis, count, by):
        return lax.ppermute(array, axis, [(n, (n + by) % count) for n in range(count)])

    half_way = fs_count // 2
    reach = [(half_way, fs_count - 1 - half_way), (fs_count - 1 - half_way, half_way)]

    rows_here, cols_here = up_weight.shape
    sub_rows = rows_here // group_count
    folded = (norm_gain[:, None] * up_weight).astype(jnp.bfloat16)
    group_pieces = []
    for k in range(group_count):
        mine = lax.dynamic_slice_in_dim(folded, ((c + k) % group_count) * sub_rows, sub_rows, 0)
        group_pieces.append(mine if k == 0 else shift(mine, ("gr", "tp"), group_count, k))
    stack = jnp.stack(group_pieces)

    token_count, features_here = tokens.shape
    half = token_count // 2
    gathered = []
    for h in range(2):
        own = tokens[h * half : (h + 1) * half]
        parts = [(own, 0, half, 0, f * features_here)]
        for sign, steps in zip((1, -1), reach[h]):
            moving = own
            for k in range(1, steps + 1):
                moving = ring_shift(moving, sign)
                parts.append((moving, 0, half, 0, at_ring(-sign * k) * features_here))
        gathered.append(parts)

    unit_width = cols_here * group_count // fs_count
    units_in_group = cols_here // unit_width
    unit_pieces = []
    for k in range(fs_count):
        unit = (f + k) % fs_count
        held = (c - unit // units_in_group) % group_count
        block = lax.dynamic_slice(
            stack, (held, 0, (unit % units_in_group) * unit_width), (1, sub_rows, unit_width)
        )[0]
        unit_pieces.append(block if k == 0 else shift(block, "fs", fs_count, k))

    down_cast = down_weight.astype(jnp.bfloat16)
    down_cast, _ = lax.optimization_barrier((down_cast, group_pieces[-1]))
    down_rows, down_cols = down_cast.shape
    down_parts = []
    for i in range(gr_count):
        over_gr = down_cast if i == 0 else shift(down_cast, "gr", gr_count, i)
        for j in range(tp_count):
            over_tp = over_gr if j == 0 else shift(over_gr, "tp", tp_count, j)
            source = ((g - i) % gr_count) * tp_count + (t - j) % tp_count
            down_parts.append((over_tp, 0, down_rows, 0, source * down_cols))
    down_full = place((down_rows, down_cols * group_count), down_parts)

    up_parts = []
    batch = fs_count // 2
    for start in range(0, fs_count, batch):
        ks = range(start, start + batch)
        joined = jnp.concatenate([unit_pieces[k] for k in ks])
        for i in range(gr_count):
            over_gr = joined if i == 0 else shift(joined, "gr", gr_count, i)
            for j in range(tp_count):
                over_tp = over_gr if j == 0 else shift(over_gr, "tp", tp_count, j)
                source = ((g - i) % gr_count) * tp_count + (t - j) % tp_count
                for n, k in enumerate(ks):
                    row = ((f - k) % fs_count) * rows_here + source * sub_rows
                    up_parts.append((over_tp, n * sub_rows, sub_rows, row, 0))
    model_width = rows_here * fs_count
    up_full = place((model_width, unit_width), up_parts)

    out_rows = down_full.shape[1] // fs_count
    outcome = []
    for h in range(2):
        piece = place((half, model_width), gathered[h])
        piece_wide = piece.astype(jnp.float32)
        row_scale = lax.rsqrt(jnp.sum(piece_wide * piece_wide, axis=1) / model_width + epsilon)
        raw_up = jnp.dot(piece, up_full, preferred_element_type=jnp.float32)
        hidden = jnp.square(jax.nn.relu(raw_up * row_scale[:, None])).astype(jnp.bfloat16)

        def partial(shift_by):
            weight = lax.dynamic_slice_in_dim(down_full, at_ring(shift_by) * out_rows, out_rows, 1)
            return lax.dot_general(weight, hidden, (((0,), (1,)), ((), ())), preferred_element_type=jnp.float32)

        arrived = []
        for sign, steps in zip((1, -1), reach[h]):
            moving = None
            for s in range(steps, 0, -1):
                here = partial(sign * s)
                if moving is not None:
                    here = here + moving.astype(jnp.float32)
                moving = ring_shift(here.astype(jnp.bfloat16), sign)
            if moving is not None:
                arrived.append(moving)
        total = partial(0)
        for moving in arrived:
            total = total + moving.astype(jnp.float32)
        outcome.append(total.astype(jnp.bfloat16))
    return (jnp.concatenate(outcome, axis=1), up_full, down_full)


def solution(mesh):
    in_specs = (P(("gr", "tp"), "fs"), P("fs"), P("fs", ("gr", "tp")), P("fs", ("gr", "tp")))
    out_specs = (P("fs", ("gr", "tp")), P(None, "fs"), P("fs", None))
    return jax.shard_map(shards, mesh=mesh, in_specs=in_specs, out_specs=out_specs, check_vma=False)
```

```python
import math

import jax
import jax.numpy as jnp
from jax import lax
from jax.experimental import pallas as pl
from jax.experimental.pallas import tpu as pltpu
from jax.sharding import PartitionSpec as P

epsilon = 1e-06


def ring_order(count):
    outer = math.gcd(count, 4)
    inner = count // outer
    if outer % 2 or inner < 2:
        return list(range(count))
    walk = []
    for o in range(outer):
        cols = range(1, inner) if o % 2 == 0 else range(inner - 1, 0, -1)
        walk += [o * inner + i for i in cols]
    return walk + [o * inner for o in range(outer - 1, -1, -1)]


def pick(index, table):
    chosen = jnp.int32(table[0])
    for n in range(1, len(table)):
        chosen = jnp.where(index == n, jnp.int32(table[n]), chosen)
    return chosen


def places():
    return lax.axis_index("fs"), lax.axis_index("gr"), lax.axis_index("tp")


def place(shape, parts):
    arrays, index_of = [], {}
    for part in parts:
        if id(part[0]) not in index_of:
            index_of[id(part[0])] = len(arrays)
            arrays.append(part[0])
    dtype = arrays[0].dtype

    def value(offset):
        return offset(*places()) if callable(offset) else offset

    if any(p[2] % 16 or p[1] % 16 or p[0].shape[1] % 128 for p in parts):
        out = jnp.zeros(shape, dtype)
        for array, source, rows, row, col in parts:
            out = lax.dynamic_update_slice(out, array[source : source + rows], (value(row), value(col)))
        return out

    def kernel(*refs):
        out_ref = refs[-1]
        for array, source, rows, row, col in parts:
            row, col = value(row), value(col)
            row = row if isinstance(row, int) else pl.multiple_of(row, 16)
            col = col if isinstance(col, int) else pl.multiple_of(col, 128)
            out_ref[pl.ds(row, rows), pl.ds(col, array.shape[1])] = refs[index_of[id(array)]][source : source + rows, :]

    whole = pl.BlockSpec(memory_space=pltpu.VMEM)
    return pl.pallas_call(
        kernel,
        out_shape=jax.ShapeDtypeStruct(shape, dtype),
        in_specs=[whole] * len(arrays),
        out_specs=whole,
    )(*arrays)


def shards(tokens, norm_gain, up_weight, down_weight):
    fs_count = lax.axis_size("fs")
    gr_count, tp_count = lax.axis_size("gr"), lax.axis_size("tp")
    group_count = gr_count * tp_count
    f, g, t = lax.axis_index("fs"), lax.axis_index("gr"), lax.axis_index("tp")
    c = g * tp_count + t
    order = ring_order(fs_count)

    def at_ring(shift_by, position):
        return pick(position, [order[(order.index(n) + shift_by) % fs_count] for n in range(fs_count)])

    def ring_shift(array, by):
        return lax.ppermute(array, "fs", [(order[n], order[(n + by) % fs_count]) for n in range(fs_count)])

    def shift(array, axis, count, by):
        return lax.ppermute(array, axis, [(n, (n + by) % count) for n in range(count)])

    def group_source(i, j):
        return lambda g, t: ((g + gr_count - i) % gr_count) * tp_count + (t + tp_count - j) % tp_count

    half_way = fs_count // 2
    reach = [(half_way, fs_count - 1 - half_way), (fs_count - 1 - half_way, half_way)]

    rows_here, cols_here = up_weight.shape
    sub_rows = rows_here // group_count
    folded = (norm_gain[:, None] * up_weight).astype(jnp.bfloat16)
    group_pieces = []
    for k in range(group_count):
        mine = lax.dynamic_slice_in_dim(folded, ((c + k) % group_count) * sub_rows, sub_rows, 0)
        group_pieces.append(mine if k == 0 else shift(mine, ("gr", "tp"), group_count, k))
    stack = jnp.stack(group_pieces)

    token_count, features_here = tokens.shape
    half = token_count // 2

    def token_part(array, row, shift_by):
        return (array, 0, array.shape[0], row, lambda f, g, t: at_ring(shift_by, f) * features_here)

    token_parts = [token_part(tokens, 0, 0)]
    before, after = tokens, tokens
    for k in range(1, (fs_count + 1) // 2):
        before, after = ring_shift(before, 1), ring_shift(after, -1)
        token_parts += [token_part(before, 0, -k), token_part(after, 0, k)]
    if fs_count % 2 == 0:
        token_parts.append(token_part(ring_shift(before[:half], 1), 0, half_way))
        token_parts.append(token_part(ring_shift(after[half:], -1), half, half_way))

    unit_width = cols_here * group_count // fs_count
    units_in_group = cols_here // unit_width
    unit_pieces = []
    for k in range(fs_count):
        unit = (f + k) % fs_count
        held = (c - unit // units_in_group) % group_count
        block = lax.dynamic_slice(
            stack, (held, 0, (unit % units_in_group) * unit_width), (1, sub_rows, unit_width)
        )[0]
        unit_pieces.append(block if k == 0 else shift(block, "fs", fs_count, k))

    down_cast = down_weight.astype(jnp.bfloat16)
    down_cast, _ = lax.optimization_barrier((down_cast, group_pieces[-1]))
    down_rows, down_cols = down_cast.shape
    down_parts = []
    for i in range(gr_count):
        over_gr = down_cast if i == 0 else shift(down_cast, "gr", gr_count, i)
        for j in range(tp_count):
            over_tp = over_gr if j == 0 else shift(over_gr, "tp", tp_count, j)
            source = group_source(i, j)
            down_parts.append((over_tp, 0, down_rows, 0, lambda f, g, t, source=source: source(g, t) * down_cols))
    down_full = place((down_rows, down_cols * group_count), down_parts)

    up_parts = []
    batch = fs_count // 2
    for start in range(0, fs_count, batch):
        ks = range(start, start + batch)
        joined = jnp.concatenate([unit_pieces[k] for k in ks])
        for i in range(gr_count):
            over_gr = joined if i == 0 else shift(joined, "gr", gr_count, i)
            for j in range(tp_count):
                over_tp = over_gr if j == 0 else shift(over_gr, "tp", tp_count, j)
                source = group_source(i, j)
                for n, k in enumerate(ks):

                    def row(f, g, t, k=k, source=source):
                        return ((f + fs_count - k) % fs_count) * rows_here + source(g, t) * sub_rows

                    up_parts.append((over_tp, n * sub_rows, sub_rows, row, 0))
    model_width = rows_here * fs_count
    up_full = place((model_width, unit_width), up_parts)

    out_rows = down_full.shape[1] // fs_count
    token_rows = place((token_count, model_width), token_parts)
    outcome = []
    for h in range(2):
        piece = token_rows[h * half : (h + 1) * half]
        piece_wide = piece.astype(jnp.float32)
        row_scale = lax.rsqrt(jnp.sum(piece_wide * piece_wide, axis=1) / model_width + epsilon)
        raw_up = jnp.dot(piece, up_full, preferred_element_type=jnp.float32)
        hidden = jnp.square(jax.nn.relu(raw_up * row_scale[:, None])).astype(jnp.bfloat16)

        def partial(shift_by):
            weight = lax.dynamic_slice_in_dim(down_full, at_ring(shift_by, f) * out_rows, out_rows, 1)
            return lax.dot_general(weight, hidden, (((0,), (1,)), ((), ())), preferred_element_type=jnp.float32)

        arrived = []
        for sign, steps in zip((1, -1), reach[h]):
            moving = None
            for s in range(steps, 0, -1):
                here = partial(sign * s)
                if moving is not None:
                    here = here + moving.astype(jnp.float32)
                moving = ring_shift(here.astype(jnp.bfloat16), sign)
            if moving is not None:
                arrived.append(moving)
        total = partial(0)
        for moving in arrived:
            total = total + moving.astype(jnp.float32)
        outcome.append(total.astype(jnp.bfloat16))
    return (jnp.concatenate(outcome, axis=1), up_full, down_full)


def solution(mesh):
    in_specs = (P(("gr", "tp"), "fs"), P("fs"), P("fs", ("gr", "tp")), P("fs", ("gr", "tp")))
    out_specs = (P("fs", ("gr", "tp")), P(None, "fs"), P("fs", None))
    return jax.shard_map(shards, mesh=mesh, in_specs=in_specs, out_specs=out_specs, check_vma=False)
```

```python
import math

import jax
import jax.numpy as jnp
from jax import lax
from jax.experimental import pallas as pl
from jax.experimental.pallas import tpu as pltpu
from jax.sharding import PartitionSpec as P

epsilon = 1e-06


def ring_order(count):
    outer = math.gcd(count, 4)
    inner = count // outer
    if outer % 2 or inner < 2:
        return list(range(count))
    walk = []
    for o in range(outer):
        cols = range(1, inner) if o % 2 == 0 else range(inner - 1, 0, -1)
        walk += [o * inner + i for i in cols]
    return walk + [o * inner for o in range(outer - 1, -1, -1)]


def pick(index, table):
    chosen = jnp.int32(table[0])
    for n in range(1, len(table)):
        chosen = jnp.where(index == n, jnp.int32(table[n]), chosen)
    return chosen


def places():
    return lax.axis_index("fs"), lax.axis_index("gr"), lax.axis_index("tp")


def place(shape, parts):
    arrays, index_of = [], {}
    for part in parts:
        if id(part[0]) not in index_of:
            index_of[id(part[0])] = len(arrays)
            arrays.append(part[0])
    dtype = arrays[0].dtype

    def value(offset):
        return offset(*places()) if callable(offset) else offset

    if any(p[2] % 16 or p[1] % 16 or p[0].shape[1] % 128 for p in parts):
        out = jnp.zeros(shape, dtype)
        for array, source, rows, row, col in parts:
            out = lax.dynamic_update_slice(out, array[source : source + rows], (value(row), value(col)))
        return out

    def kernel(*refs):
        out_ref = refs[-1]
        for array, source, rows, row, col in parts:
            row, col = value(row), value(col)
            row = row if isinstance(row, int) else pl.multiple_of(row, 16)
            col = col if isinstance(col, int) else pl.multiple_of(col, 128)
            out_ref[pl.ds(row, rows), pl.ds(col, array.shape[1])] = refs[index_of[id(array)]][source : source + rows, :]

    whole = pl.BlockSpec(memory_space=pltpu.VMEM)
    return pl.pallas_call(
        kernel,
        out_shape=jax.ShapeDtypeStruct(shape, dtype),
        in_specs=[whole] * len(arrays),
        out_specs=whole,
    )(*arrays)


def shards(tokens, norm_gain, up_weight, down_weight):
    fs_count = lax.axis_size("fs")
    gr_count, tp_count = lax.axis_size("gr"), lax.axis_size("tp")
    group_count = gr_count * tp_count
    f, g, t = lax.axis_index("fs"), lax.axis_index("gr"), lax.axis_index("tp")
    c = g * tp_count + t
    order = ring_order(fs_count)

    def at_ring(shift_by, position):
        return pick(position, [order[(order.index(n) + shift_by) % fs_count] for n in range(fs_count)])

    def ring_shift(array, by):
        return lax.ppermute(array, "fs", [(order[n], order[(n + by) % fs_count]) for n in range(fs_count)])

    def shift(array, axis, count, by):
        return lax.ppermute(array, axis, [(n, (n + by) % count) for n in range(count)])

    def group_source(i, j):
        return lambda g, t: ((g + gr_count - i) % gr_count) * tp_count + (t + tp_count - j) % tp_count

    half_way = fs_count // 2
    reach = [(half_way, fs_count - 1 - half_way), (fs_count - 1 - half_way, half_way)]

    rows_here, cols_here = up_weight.shape
    sub_rows = rows_here // group_count
    folded = (norm_gain[:, None] * up_weight).astype(jnp.bfloat16)
    group_pieces = []
    for k in range(group_count):
        mine = lax.dynamic_slice_in_dim(folded, ((c + k) % group_count) * sub_rows, sub_rows, 0)
        group_pieces.append(mine if k == 0 else shift(mine, ("gr", "tp"), group_count, k))
    stack = jnp.stack(group_pieces)

    token_count, features_here = tokens.shape
    half = token_count // 2

    def token_part(array, row, shift_by):
        return (array, 0, array.shape[0], row, lambda f, g, t: at_ring(shift_by, f) * features_here)

    token_parts = [token_part(tokens, 0, 0)]
    before, after = tokens, tokens
    for k in range(1, (fs_count + 1) // 2):
        before, after = ring_shift(before, 1), ring_shift(after, -1)
        token_parts += [token_part(before, 0, -k), token_part(after, 0, k)]
    unit_width = cols_here * group_count // fs_count
    units_in_group = cols_here // unit_width
    unit_pieces = []
    for k in range(fs_count):
        unit = (f + k) % fs_count
        held = (c - unit // units_in_group) % group_count
        block = lax.dynamic_slice(
            stack, (held, 0, (unit % units_in_group) * unit_width), (1, sub_rows, unit_width)
        )[0]
        unit_pieces.append(block if k == 0 else shift(block, "fs", fs_count, k))

    down_cast = down_weight.astype(jnp.bfloat16)
    down_cast, _ = lax.optimization_barrier((down_cast, group_pieces[-1]))
    down_rows, down_cols = down_cast.shape
    down_parts = []
    for i in range(gr_count):
        over_gr = down_cast if i == 0 else shift(down_cast, "gr", gr_count, i)
        for j in range(tp_count):
            over_tp = over_gr if j == 0 else shift(over_gr, "tp", tp_count, j)
            source = group_source(i, j)
            down_parts.append((over_tp, 0, down_rows, 0, lambda f, g, t, source=source: source(g, t) * down_cols))
    down_full = place((down_rows, down_cols * group_count), down_parts)

    def squares_of(array):
        wide = array.astype(jnp.float32)
        return jnp.sum(wide * wide, axis=1)

    squares = sum(squares_of(part[0]) for part in token_parts)
    last = None
    if fs_count % 2 == 0:
        token_parts.append(token_part(jnp.zeros_like(tokens), 0, half_way))
    token_rows = place((token_count, features_here * fs_count), token_parts)
    down_full, squares, token_rows = lax.optimization_barrier((down_full, squares, token_rows))
    if fs_count % 2 == 0:
        last = (ring_shift(before[:half], 1), ring_shift(after[half:], -1))

    up_parts = []
    batch = fs_count // 2
    for start in range(0, fs_count, batch):
        ks = range(start, start + batch)
        joined = jnp.concatenate([unit_pieces[k] for k in ks])
        for i in range(gr_count):
            over_gr = joined if i == 0 else shift(joined, "gr", gr_count, i)
            for j in range(tp_count):
                over_tp = over_gr if j == 0 else shift(over_gr, "tp", tp_count, j)
                source = group_source(i, j)
                for n, k in enumerate(ks):

                    def row(f, g, t, k=k, source=source):
                        return ((f + fs_count - k) % fs_count) * rows_here + source(g, t) * sub_rows

                    up_parts.append((over_tp, n * sub_rows, sub_rows, row, 0))
    model_width = rows_here * fs_count
    up_full = place((model_width, unit_width), up_parts)

    out_rows = down_full.shape[1] // fs_count
    outcome = []
    for h in range(2):
        piece = token_rows[h * half : (h + 1) * half]
        raw_up = jnp.dot(piece, up_full, preferred_element_type=jnp.float32)
        squares_here = squares[h * half : (h + 1) * half]
        if last is not None:
            last_rows = lax.dynamic_slice_in_dim(up_full, at_ring(half_way, f) * rows_here, rows_here, 0)
            raw_up = raw_up + jnp.dot(last[h], last_rows, preferred_element_type=jnp.float32)
            squares_here = squares_here + squares_of(last[h])
        row_scale = lax.rsqrt(squares_here / model_width + epsilon)
        hidden = jnp.square(jax.nn.relu(raw_up * row_scale[:, None])).astype(jnp.bfloat16)

        def partial(shift_by):
            weight = lax.dynamic_slice_in_dim(down_full, at_ring(shift_by, f) * out_rows, out_rows, 1)
            return lax.dot_general(weight, hidden, (((0,), (1,)), ((), ())), preferred_element_type=jnp.float32)

        arrived = []
        for sign, steps in zip((1, -1), reach[h]):
            moving = None
            for s in range(steps, 0, -1):
                here = partial(sign * s)
                if moving is not None:
                    here = here + moving.astype(jnp.float32)
                moving = ring_shift(here.astype(jnp.bfloat16), sign)
            if moving is not None:
                arrived.append(moving)
        total = partial(0)
        for moving in arrived:
            total = total + moving.astype(jnp.float32)
        outcome.append(total.astype(jnp.bfloat16))
    return (jnp.concatenate(outcome, axis=1), up_full, down_full)


def solution(mesh):
    in_specs = (P(("gr", "tp"), "fs"), P("fs"), P("fs", ("gr", "tp")), P("fs", ("gr", "tp")))
    out_specs = (P("fs", ("gr", "tp")), P(None, "fs"), P("fs", None))
    return jax.shard_map(shards, mesh=mesh, in_specs=in_specs, out_specs=out_specs, check_vma=False)
```
